32 devices in a mesh: fs: 8 (over z, y), tp: 4 (over x, core).
Axes of the slice: x: 2, y: 2, z: 4, core: 2. Of those that a mesh axis runs over, the one named last changes fastest.
Arguments:
- tokens: bfloat16 [4096, 2048], P(('fs', 'tp')), may hold values from -6 to 6
- pre_gain: float32 [2048], replicated, may hold values from 0.1 to 1.9
- w_expand: bfloat16 [2048, 8192], P('fs', 'tp'), may hold values from -0.125 to 0.125
- w_reduce: bfloat16 [8192, 2048], P('tp', 'fs'), may hold values from -0.0625 to 0.0625
- post_gain: float32 [2048], replicated, may hold values from 0.1 to 1.9
Outputs:
- result: bfloat16 [4096, 2048], P(('fs', 'tp'))
The draws below stay inside these ranges and needn't reach their ends.
All inputs are finite; a program needn't handle non-finite values.
Results may differ from the reference program's by a relative error of at most 0.014.
Values may be sent and summed in bfloat16 or wider, within the bound.
A program may use at most 64 MiB of HBM per device.

```python
import math
import jax
import jax.numpy as jnp
from jax import lax

D = 2048
FF = 8192
TOKENS = 4096
N_TP = 4


def block_levels(key, shape, cuts, low, top_value):
    level, own = 1.0, jax.random.fold_in(key, 6)
    for dim, parts in cuts:
        draws = jnp.exp(jax.random.uniform(jax.random.fold_in(own, dim), (parts,), jnp.float32, low / len(cuts), top_value / len(cuts)))
        level = level * jnp.repeat(draws, shape[dim] // parts).reshape([-1 if axis == dim else 1 for axis in range(len(shape))])
    return level


def centred(key, extent, deviation, reach, shards=(), held_as=jnp.bfloat16):
    drawn = jax.random.normal(key, extent, jnp.float32) * deviation
    if len(shards) > 0:
        drawn = block_levels(key, extent, shards, -0.22, 0.18) * drawn
    return jnp.clip(drawn, min=-reach, max=reach).astype(held_as)


def setup_inputs(seed: int = 0) -> dict:
    key_list = jax.random.split(jax.random.key(seed), 6)
    return {
        "tokens": centred(key_list[0], (TOKENS, D), 1.0, 6.0, ((0, 32),)),
        "pre_gain": jnp.clip(1.0 + 0.18 * jax.random.normal(key_list[1], (D,), jnp.float32), 0.1, 1.9),
        "w_expand": centred(key_list[2], (D, FF), D ** -0.5, 0.125, ((0, 8), (1, 4))),
        "w_reduce": centred(key_list[3], (FF, D), FF ** -0.5, 0.0625, ((0, 4), (1, 8))),
        "post_gain": jnp.clip(1.0 + 0.18 * jax.random.normal(key_list[4], (D,), jnp.float32), 0.1, 1.9),
    }


NORM_EPS = 1e-06

def rms_scale(values, gain_row):
    widened = values.astype(jnp.float32)
    scaled = widened * lax.rsqrt(lax.optimization_barrier(jnp.mean(widened * widened, axis=-1, keepdims=True)) + NORM_EPS)
    return scaled * gain_row.astype(jnp.float32)

def reference(tokens, pre_gain, w_expand, w_reduce, post_gain):
    row_count = tokens.shape[0]
    block_rows = math.gcd(row_count, 2048)
    blocks = tokens.reshape(row_count // block_rows, block_rows, D)
    hidden_block = FF // N_TP

    def per_block(block):
        normed = rms_scale(block, pre_gain).astype(jnp.bfloat16)
        preact = jnp.dot(normed, w_expand, preferred_element_type=jnp.float32)
        hidden = jnp.square(jnp.maximum(preact, 0.0)).astype(jnp.bfloat16)
        running = jnp.zeros((block_rows, D), jnp.float32)
        for member in range(N_TP):
            partial_value = jnp.dot(hidden[:, member * hidden_block:(member + 1) * hidden_block], w_reduce[member * hidden_block:(member + 1) * hidden_block], preferred_element_type=jnp.float32).astype(jnp.bfloat16)
            partial_value = lax.optimization_barrier(partial_value)
            running = running + partial_value.astype(jnp.float32)
        mixed = running.astype(jnp.bfloat16)
        return rms_scale(mixed, post_gain).astype(jnp.bfloat16)
    return lax.map(per_block, blocks).reshape(row_count, D)
```

```python
import functools

import jax
import jax.numpy as jnp
from jax import lax
from jax.experimental import pallas as pl
from jax.experimental.pallas import tpu as pltpu
from jax.sharding import PartitionSpec as P

NORM_EPS = 1e-06
MESH = pl.DeviceIdType.MESH
TS = 2


def kernel(NX, NY, NZ, EARLY, tok, gain_in, w_e, w_r, gain_out, out,
           TG, N, WE, WR, H, O, PR, RX,
           t_ls, t_ps, t_r, e_a, e_b, e_c, e_l, e_r, r_a, r_b, r_c, r_l, r_r, p_s, p_r, c_s, c_r):
    R, D = tok.shape
    DK, F = w_e.shape
    H4 = F // NZ
    RT = R // TS
    fs, tp = lax.axis_index("fs"), lax.axis_index("tp")
    z, y = fs // NY, fs % NY
    x, c = tp // 2, tp % 2
    pc = 1 - c
    peer = (fs, x * 2 + pc)

    def zdev(q):
        return (q * NY + y, tp)

    xs = [(x + j) % NX for j in range(1, NX)]
    ys = [(y + j) % NY for j in range(1, NY)]
    xdevs = [(fs, q * 2 + c) for q in xs]
    ydevs = [(z * NY + q, tp) for q in ys]

    barrier = pltpu.get_barrier_semaphore()
    others = [zdev((z + j) % NZ) for j in range(1, NZ)] + xdevs + ydevs + [peer]
    for dev in others:
        pl.semaphore_signal(barrier, inc=1, device_id=dev, device_id_type=MESH)
    pl.semaphore_wait(barrier, len(others))

    def rc(src, dst, ss, rs, dev):
        return pltpu.make_async_remote_copy(src_ref=src, dst_ref=dst, send_sem=ss, recv_sem=rs,
                                            device_id=dev, device_id_type=MESH)

    def guarded(cond, fn):
        if cond is None:
            fn()
        else:
            pl.when(cond)(fn)

    def landed(ref, sem):
        pltpu.make_async_copy(ref, ref, sem).wait()

    def at_distance(d):
        if d == 0:
            return [(z, 0, None)]
        return [(z - d, -1, z - d >= 0), (z + d, 1, z + d < NZ)]

    def rows_of(start, size, half):
        if half is None:
            return pl.ds(pl.multiple_of(start, size), size)
        return pl.ds(pl.multiple_of(start + half * (size // 2), size // 2), size // 2)

    def e_view(xq, zq, yq, half=None):
        return WE.at[xq, rows_of((zq * NY + yq) * DK, DK, half)]

    def r_view(xq, zq, yq, half=None):
        return WR.at[zq * NY + yq, rows_of(xq * H4, H4, half)]

    def e_piece(q):
        return w_e.at[:, pl.ds(pl.multiple_of(q * H4, H4), H4)]

    def r_piece(q):
        return w_r.at[pl.ds(pl.multiple_of(q * H4, H4), H4)]

    class Weight:
        def __init__(self, view, piece, a, b, cc, l, r):
            self.view, self.piece, self.a, self.b, self.c, self.l, self.r = view, piece, a, b, cc, l, r

    E = Weight(e_view, e_piece, e_a, e_b, e_c, e_l, e_r)
    W = Weight(r_view, r_piece, r_a, r_b, r_c, r_l, r_r)
    ways = ((xdevs, xs, ydevs, ys), (ydevs, ys, xdevs, xs))

    def along_line(w, d):
        for q, s, ok in at_distance(d):
            guarded(ok, lambda q=q: rc(w.piece(q), w.view(x, z, y), w.a.at[q], w.l.at[z], zdev(q)).start())

    def first(w, q):
        landed(w.view(x, q, y), w.l.at[q])
        for h in (0, 1):
            for j, dev in enumerate(ways[h][0]):
                rc(w.view(x, q, y, h), w.view(x, q, y, h), w.b.at[q, j, h], w.r.at[x, q, y, h], dev).start()
        for h in (0, 1):
            for j, dev in enumerate(ways[h][2]):
                rc(w.view(x, q, y, h), w.view(x, q, y, h), w.c.at[q, 0, j, h], w.r.at[x, q, y, h], dev).start()

    def second(w, q):
        for h in (0, 1):
            for i, m in enumerate(ways[h][1]):
                where = (m, q, y) if h == 0 else (x, q, m)
                landed(w.view(*where, h), w.r.at[(*where, h)])
                for j, dev in enumerate(ways[h][2]):
                    rc(w.view(*where, h), w.view(*where, h), w.c.at[q, 1 + i, j, h], w.r.at[(*where, h)], dev).start()

    def last(w, q):
        for h in (0, 1):
            for a in [x] + xs if h == 0 else xs:
                for b in ys if h == 0 else [y] + ys:
                    landed(w.view(a, q, b, h), w.r.at[a, q, b, h])

    def both(fn, w, d):
        for q, s, ok in at_distance(d):
            guarded(ok, lambda q=q: fn(w, q))

    def drain_weight(w):
        def body(q, carry):
            pl.when(q != z)(lambda: rc(w.piece(q), w.view(x, z, y), w.a.at[q], w.l.at[z], peer).wait_send())
            for h in (0, 1):
                v = w.view(x, q, y, h)
                for j in range(len(ways[h][0])):
                    rc(v, v, w.b.at[q, j, h], w.r.at[x, q, y, h], peer).wait_send()
                for i in range(1 + len(ways[h][1])):
                    for j in range(len(ways[h][2])):
                        rc(v, v, w.c.at[q, i, j, h], w.r.at[x, q, y, h], peer).wait_send()
            return carry

        lax.fori_loop(0, NZ, body, 0)

    def t_view(q, cc, u):
        return TG.at[q, cc, pl.ds(u * RT, RT)]

    def send_tokens(src, q, u, n, side, ok):
        guarded(ok, lambda: rc(src, t_view(q, c, u), t_ls.at[q, side, u], t_r.at[q, c, u], zdev(n)).start())

    def peer_tokens(src, q, u, ok):
        guarded(ok, lambda: rc(src, t_view(q, c, u), t_ps.at[q, u], t_r.at[q, c, u], peer).start())

    def tokens_step(d):
        for u in range(TS):
            for q, s, ok in at_distance(d):
                guarded(ok, lambda q=q, u=u: landed(t_view(q, c, u), t_r.at[q, c, u]))
                n = z - s
                send_tokens(t_view(q, c, u), q, u, n, (1 - s) // 2,
                            jnp.logical_and(ok, jnp.logical_and(n >= 0, n < NZ)))
                peer_tokens(t_view(q, c, u), q, u, ok)

    M = 2 * R
    sub = 32

    def norm_rows(q):
        for u in range(TS):
            landed(t_view(q, pc, u), t_r.at[q, pc, u])
        base = q * M if EARLY else 0

        def norm(i, carry):
            v = TG[q, i // (R // sub), pl.ds(pl.multiple_of((i % (R // sub)) * sub, sub), sub)].astype(jnp.float32)
            v = v * lax.rsqrt(jnp.mean(v * v, axis=-1, keepdims=True) + NORM_EPS) * gain_in[...]
            N[pl.ds(pl.multiple_of(base + i * sub, sub), sub)] = v.astype(jnp.bfloat16)
            return carry

        lax.fori_loop(0, M // sub, norm, 0)

    def expand_rows(q, carry):
        if not EARLY:
            norm_rows(q)
        rows = pl.ds(pl.multiple_of(q * M, M), M)
        src = rows if EARLY else slice(None)
        for i in range(NX):
            p = jnp.dot(N[src], WE[i], preferred_element_type=jnp.float32)
            H[rows, i * H4:(i + 1) * H4] = jnp.square(jnp.maximum(p, 0.0)).astype(jnp.bfloat16)
        return carry

    def norm_at(d):
        if EARLY:
            for q, s, ok in at_distance(d):
                guarded(ok, lambda q=q: norm_rows(q))

    big = 2 * M if NZ % 2 == 0 else M
    nb = NZ * M // big

    def columns(g):
        def body(k, carry):
            f, i = g * NY + k // nb, k % nb
            p = jnp.dot(H[pl.ds(pl.multiple_of(i * big, big), big)], WR[f], preferred_element_type=jnp.float32)
            O[pl.ds(i * (big // M), big // M), :, f] = p.astype(jnp.bfloat16).reshape(big // M, 2, R, DK)
            return carry

        lax.fori_loop(0, NY * nb, body, 0)

    def part(g):
        return pl.ds(g * NY, NY)

    def pair_copy(g):
        return rc(O.at[:, pc, part(g)], PR.at[:, part(g)], p_s.at[g], p_r.at[g], peer)

    def pass_on(q, g, slot, n):
        return rc(O.at[q, c, part(g)], RX.at[slot, part(g)], c_s.at[q, g], c_r.at[slot, g], zdev(n))

    def add_part(q, g, slots):
        for slot in slots:
            landed(RX.at[slot, part(g)], c_r.at[slot, g])

        def body(f, carry):
            s = O[q, c, f].astype(jnp.float32) + PR[q, f].astype(jnp.float32)
            for slot in slots:
                s += RX[slot, f].astype(jnp.float32)
            O[q, c, f] = s.astype(jnp.bfloat16)
            return carry

        lax.fori_loop(g * NY, (g + 1) * NY, body, 0)

    def flow(g, right):
        for j in range(NZ - 1):
            q = NZ - 1 - j if right else j
            n = z + 1 if right else z - 1
            ok = q > z if right else q < z
            has = z > 0 if right else z < NZ - 1
            slot = jnp.where(q == n, NZ, q) if right else q

            def step(q=q, n=n, slot=slot, has=has):
                pl.when(has)(lambda: add_part(q, g, [q]))
                pl.when(jnp.logical_not(has))(lambda: add_part(q, g, []))
                pass_on(q, g, slot, n).start()

            pl.when(ok)(step)

    def column_block(g):
        last(W, g)
        columns(g)
        pair_copy(g).start()

    def pair_in(g):
        landed(PR.at[:, part(g)], p_r.at[g])

    def stage(t):
        if t < NZ:
            for q, s, ok in at_distance(t):
                guarded(ok, lambda q=q: column_block(q))
        if 1 <= t <= NZ:
            for q, s, ok in at_distance(t - 1):
                guarded(ok, lambda q=q: pair_in(q))
        for right, hops in ((True, z), (False, NZ - 1 - z)):
            k = t - 1 - hops
            g = k if right else NZ - 1 - k
            pl.when(jnp.logical_and(k >= 0, k < NZ))(lambda g=g, right=right: flow(g, right))
        if t + 1 < NZ:
            both(second, W, t + 1)
        if t + 2 < NZ:
            both(first, W, t + 2)

    own = [pltpu.make_async_copy(t_src, t_view(z, c, u), t_r.at[z, c, u])
           for u, t_src in ((u, tok.at[pl.ds(u * RT, RT)]) for u in range(TS))]
    own += [pltpu.make_async_copy(E.piece(z), E.view(x, z, y), E.l.at[z]),
            pltpu.make_async_copy(W.piece(z), W.view(x, z, y), W.l.at[z])]
    for copy in own:
        copy.start()
    for u in range(TS):
        src = tok.at[pl.ds(u * RT, RT)]
        send_tokens(src, z, u, z - 1, 0, z >= 1)
        send_tokens(src, z, u, z + 1, 1, z + 1 < NZ)
        peer_tokens(src, z, u, None)
    along_line(E, 1)
    first(E, z)
    for d in range(2, NZ):
        along_line(E, d)
    first(W, z)
    second(E, z)
    for u in range(TS):
        landed(t_view(z, c, u), t_r.at[z, c, u])
    norm_at(0)
    tokens_step(1)
    second(W, z)
    both(first, E, 1)
    both(second, E, 1)
    for d in range(2, NZ):
        tokens_step(d)
        both(first, E, d)
        norm_at(d - 1)
        both(second, E, d)
    for d in range(1, NZ):
        along_line(W, d)
    norm_at(NZ - 1)
    for d in range(NZ):
        both(last, E, d)
    lax.fori_loop(0, NZ, expand_rows, 0)
    if NZ > 1:
        both(first, W, 1)
    for t in range(2 * NZ):
        stage(t)

    def finish(g, carry):
        pl.when(jnp.logical_and(z > 0, z < NZ - 1))(lambda: add_part(z, g, [z, NZ]))
        pl.when(z == 0)(lambda: add_part(z, g, [z]))
        pl.when(z == NZ - 1)(lambda: add_part(z, g, [NZ]))
        return carry

    lax.fori_loop(0, NZ, finish, 0)

    def squares(f, acc):
        m = O[z, c, f].astype(jnp.float32)
        return acc + jnp.sum(m * m, axis=-1, keepdims=True)

    total = lax.fori_loop(0, NZ * NY, squares, jnp.zeros((R, 1), jnp.float32))
    scale = lax.rsqrt(total / D + NORM_EPS)
    for f in range(NZ * NY):
        cols = slice(f * DK, (f + 1) * DK)
        out[:, cols] = (O[z, c, f].astype(jnp.float32) * scale * gain_out[:, cols]).astype(jnp.bfloat16)

    drain_weight(E)
    drain_weight(W)

    def drain(q, carry):
        for u in range(TS):
            v = t_view(q, c, u)
            rc(v, v, t_ps.at[q, u], t_r.at[q, c, u], peer).wait_send()
            pl.when(jnp.logical_and(q >= z, z >= 1))(
                lambda: rc(v, v, t_ls.at[q, 0, u], t_r.at[q, c, u], peer).wait_send())
            pl.when(jnp.logical_and(q <= z, z < NZ - 1))(
                lambda: rc(v, v, t_ls.at[q, 1, u], t_r.at[q, c, u], peer).wait_send())
        pair_copy(q).wait_send()
        for g in range(NZ):
            pl.when(q != z)(lambda: pass_on(q, g, q, z).wait_send())
        return carry

    lax.fori_loop(0, NZ, drain, 0)


def per_device(FS, TP, tokens, pre_gain, w_expand, w_reduce, post_gain):
    NX = TP // 2
    NY = max(k for k in range(1, FS + 1) if FS % k == 0 and (k == 1 or 2 * k * k <= FS))
    NZ = FS // NY
    R, D = tokens.shape
    DK, F = w_expand.shape
    H4 = F // NZ
    bf = jnp.bfloat16
    dma = pltpu.SemaphoreType.DMA
    mx = max(NX, NY)
    early = 2 * NZ * R * D * 2 <= 8 * 1024 * 1024
    vmem = pl.BlockSpec(memory_space=pltpu.VMEM)
    hbm = pl.BlockSpec(memory_space=pl.ANY)
    return pl.pallas_call(
        functools.partial(kernel, NX, NY, NZ, early),
        out_shape=jax.ShapeDtypeStruct((R, D), bf),
        in_specs=[hbm, vmem, hbm, hbm, vmem],
        out_specs=vmem,
        scratch_shapes=[
            pltpu.VMEM((NZ, 2, R, D), bf),
            pltpu.VMEM(((NZ if early else 1) * 2 * R, D), bf),
            pltpu.VMEM((NX, D, H4), bf),
            pltpu.VMEM((FS, NX * H4, DK), bf),
            pltpu.VMEM((NZ * 2 * R, NX * H4), bf),
            pltpu.VMEM((NZ, 2, FS, R, DK), bf),
            pltpu.VMEM((NZ, FS, R, DK), bf),
            pltpu.VMEM((NZ + 1, FS, R, DK), bf),
            dma((NZ, 2, TS)), dma((NZ, TS)), dma((NZ, 2, TS)),
            dma((NZ,)), dma((NZ, mx, 2)), dma((NZ, mx, mx, 2)), dma((NZ,)), dma((NX, NZ, NY, 2)),
            dma((NZ,)), dma((NZ, mx, 2)), dma((NZ, mx, mx, 2)), dma((NZ,)), dma((NX, NZ, NY, 2)),
            dma((NZ,)), dma((NZ,)), dma((NZ, NZ)), dma((NZ + 1, NZ)),
        ],
        compiler_params=pltpu.CompilerParams(
            collective_id=0, has_side_effects=True, vmem_limit_bytes=64 * 1024 * 1024 - 128 * 1024),
    )(tokens, pre_gain.reshape(1, D), w_expand, w_reduce, post_gain.reshape(1, D))


def solution(mesh):
    return jax.shard_map(
        functools.partial(per_device, mesh.shape["fs"], mesh.shape["tp"]),
        mesh=mesh,
        in_specs=(P(("fs", "tp"), None), P(), P("fs", "tp"), P("tp", "fs"), P()),
        out_specs=P(("fs", "tp"), None),
        check_vma=False,
    )
```

```python
import functools

import jax
import jax.numpy as jnp
from jax import lax
from jax.experimental import pallas as pl
from jax.experimental.pallas import tpu as pltpu
from jax.sharding import PartitionSpec as P

NORM_EPS = 1e-06
MESH = pl.DeviceIdType.MESH
TS = 2


def kernel(NX, NY, NZ, EARLY, tok, gain_in, w_e, w_r, gain_out, out,
           TG, N, WE, WR, XE, XR, H, O, PR, RX,
           t_ls, t_ps, t_r, e_a, e_b, e_c, e_l, e_r, e_x, e_y, r_a, r_b, r_c, r_l, r_r, r_x, r_y, p_s, p_r, c_s, c_r):
    R, D = tok.shape
    DK, F = w_e.shape
    H4 = F // NZ
    RT = R // TS
    fs, tp = lax.axis_index("fs"), lax.axis_index("tp")
    z, y = fs // NY, fs % NY
    x, c = tp // 2, tp % 2
    pc = 1 - c
    peer = (fs, x * 2 + pc)

    low = 2 * z < NZ
    mz = jnp.where(low, z, NZ - 1 - z)
    toward = jnp.where(low, 1, -1)
    lifts = c == jnp.where(low, 1, 0)

    def src(m):
        return jnp.where(low, m, NZ - 1 - m)

    def zdev(q):
        return (q * NY + y, tp)

    xs = [(x + j) % NX for j in range(1, NX)]
    ys = [(y + j) % NY for j in range(1, NY)]
    xdevs = [(fs, q * 2 + c) for q in xs]
    ydevs = [(z * NY + q, tp) for q in ys]

    barrier = pltpu.get_barrier_semaphore()
    others = [zdev((z + j) % NZ) for j in range(1, NZ)] + xdevs + ydevs + [peer]
    for dev in others:
        pl.semaphore_signal(barrier, inc=1, device_id=dev, device_id_type=MESH)
    pl.semaphore_wait(barrier, len(others))

    def rc(src, dst, ss, rs, dev):
        return pltpu.make_async_remote_copy(src_ref=src, dst_ref=dst, send_sem=ss, recv_sem=rs,
                                            device_id=dev, device_id_type=MESH)

    def landed(ref, sem):
        pltpu.make_async_copy(ref, ref, sem).wait()

    def rows_of(start, size, half):
        if half is None:
            return pl.ds(pl.multiple_of(start, size), size)
        return pl.ds(pl.multiple_of(start + half * (size // 2), size // 2), size // 2)

    def e_view(xq, zq, yq, half=None):
        return WE.at[xq, rows_of((zq * NY + yq) * DK, DK, half)]

    def r_view(xq, zq, yq, half=None):
        return WR.at[zq * NY + yq, rows_of(xq * H4, H4, half)]

    def e_piece(q, half=None):
        cols = pl.ds(pl.multiple_of(q * H4, H4), H4)
        return w_e.at[:, cols] if half is None else w_e.at[rows_of(0, DK, half), cols]

    def r_piece(q, half=None):
        return w_r.at[rows_of(q * H4, H4, half)]

    class Weight:
        def __init__(self, view, piece, held, a, b, cc, l, r, sx, rx):
            self.view, self.piece, self.held, self.a, self.b, self.c = view, piece, held, a, b, cc
            self.l, self.r, self.sx, self.rx = l, r, sx, rx

    E = Weight(e_view, e_piece, XE, e_a, e_b, e_c, e_l, e_r, e_x, e_y)
    W = Weight(r_view, r_piece, XR, r_a, r_b, r_c, r_l, r_r, r_x, r_y)
    ways = ((xdevs, xs, ydevs, ys), (ydevs, ys, xdevs, xs))

    def hand_over(w, q):
        rc(w.piece(q), w.held.at[q], w.a.at[q], w.rx.at[q], peer).start()

    def along_line(w, q):
        rc(w.piece(q), w.view(x, z, y), w.a.at[q], w.l.at[z], zdev(q)).start()
        landed(w.held.at[q], w.rx.at[q])
        rc(w.held.at[q], w.view(x, z, y), w.sx.at[q], w.l.at[z], (q * NY + y, x * 2 + pc)).start()

    def first(w, q, own=False):
        if not own:
            landed(w.view(x, q, y), w.l.at[q])
        for h in (0, 1):
            for j, dev in enumerate(ways[h][0]):
                rc(w.piece(q, h) if own else w.view(x, q, y, h), w.view(x, q, y, h), w.b.at[q, j, h],
                   w.r.at[x, q, y, h], dev).start()
        for h in (0, 1):
            for j, dev in enumerate(ways[h][2]):
                rc(w.piece(q, h) if own else w.view(x, q, y, h), w.view(x, q, y, h), w.c.at[q, 0, j, h],
                   w.r.at[x, q, y, h], dev).start()

    def second(w, q):
        for h in (0, 1):
            for i, m in enumerate(ways[h][1]):
                where = (m, q, y) if h == 0 else (x, q, m)
                landed(w.view(*where, h), w.r.at[(*where, h)])
                for j, dev in enumerate(ways[h][2]):
                    rc(w.view(*where, h), w.view(*where, h), w.c.at[q, 1 + i, j, h], w.r.at[(*where, h)], dev).start()

    def last(w, q):
        for h in (0, 1):
            for a in [x] + xs if h == 0 else xs:
                for b in ys if h == 0 else [y] + ys:
                    landed(w.view(a, q, b, h), w.r.at[a, q, b, h])

    def drain_weight(w):
        def body(q, carry):
            pl.when(q != z)(lambda: rc(w.piece(q), w.view(x, z, y), w.a.at[q], w.l.at[z], peer).wait_send())
            pl.when(jnp.where(lifts, src(q) > mz, src(q) < mz))(
                lambda: rc(w.held.at[q], w.view(x, z, y), w.sx.at[q], w.l.at[z], peer).wait_send())
            for h in (0, 1):
                v = w.view(x, q, y, h)
                for j in range(len(ways[h][0])):
                    rc(v, v, w.b.at[q, j, h], w.r.at[x, q, y, h], peer).wait_send()
                for i in range(1 + len(ways[h][1])):
                    for j in range(len(ways[h][2])):
                        rc(v, v, w.c.at[q, i, j, h], w.r.at[x, q, y, h], peer).wait_send()
            return carry

        lax.fori_loop(0, NZ, body, 0)

    def t_view(q, cc, u):
        return TG.at[q, cc, pl.ds(u * RT, RT)]

    def send_tokens(source, q, cc, u, up):
        n = z + toward if up else z - toward
        dev = (n * NY + y, tp)
        rc(source, t_view(q, cc, u), t_ls.at[q, cc, u], t_r.at[q, cc, u], dev).start()

    def peer_tokens(source, q, cc, u):
        rc(source, t_view(q, cc, u), t_ps.at[q, cc, u], t_r.at[q, cc, u], peer).start()

    def relay_tokens(k, m, up):
        q = src(m)
        for u in range(TS):
            for cc in (0, 1):
                v = t_view(q, cc, u)
                landed(v, t_r.at[q, cc, u])
                if up or k > 0:
                    send_tokens(v, q, cc, u, up)
                peer_tokens(v, q, cc, u)

    def own_tokens(k, up):
        for u in range(TS):
            peer_tokens(tok.at[pl.ds(u * RT, RT)], z, c, u)
        linked = NZ > 1 and (up or k > 0)
        if linked:
            for u in range(TS):
                send_tokens(tok.at[pl.ds(u * RT, RT)], z, c, u, up)
        for u in range(TS):
            landed(t_view(z, pc, u), t_r.at[z, pc, u])
            if linked:
                send_tokens(t_view(z, pc, u), z, pc, u, up)

    def take_tokens(q):
        for u in range(TS):
            for cc in (0, 1):
                landed(t_view(q, cc, u), t_r.at[q, cc, u])

    M = 2 * R
    sub = 32

    def norm_rows(q):
        base = q * M if EARLY else 0

        def norm(i, carry):
            v = TG[q, i // (R // sub), pl.ds(pl.multiple_of((i % (R // sub)) * sub, sub), sub)].astype(jnp.float32)
            v = v * lax.rsqrt(jnp.mean(v * v, axis=-1, keepdims=True) + NORM_EPS) * gain_in[...]
            N[pl.ds(pl.multiple_of(base + i * sub, sub), sub)] = v.astype(jnp.bfloat16)
            return carry

        lax.fori_loop(0, M // sub, norm, 0)

    def expand_rows(q):
        if not EARLY:
            norm_rows(q)
        rows = pl.ds(pl.multiple_of(q * M, M), M)
        src = rows if EARLY else slice(None)
        for i in range(NX):
            p = jnp.dot(N[src], WE[i], preferred_element_type=jnp.float32)
            H[rows, i * H4:(i + 1) * H4] = jnp.square(jnp.maximum(p, 0.0)).astype(jnp.bfloat16)

    big = 2 * M if NZ % 2 == 0 else M
    nb = NZ * M // big

    def columns(g):
        def body(k, carry):
            f, i = g * NY + k // nb, k % nb
            p = jnp.dot(H[pl.ds(pl.multiple_of(i * big, big), big)], WR[f], preferred_element_type=jnp.float32)
            O[pl.ds(i * (big // M), big // M), :, f] = p.astype(jnp.bfloat16).reshape(big // M, 2, R, DK)
            return carry

        lax.fori_loop(0, NY * nb, body, 0)

    def part(g):
        return pl.ds(g * NY, NY)

    def pair_copy(q, g):
        return rc(O.at[q, pc, part(g)], PR.at[q, part(g)], p_s.at[g, q], p_r.at[g, q], peer)

    def pass_on(q, g, slot, n):
        return rc(O.at[q, c, part(g)], RX.at[slot, part(g)], c_s.at[q, g], c_r.at[slot, g], zdev(n))

    def add_part(q, g, slots):
        landed(PR.at[q, part(g)], p_r.at[g, q])
        for slot in slots:
            landed(RX.at[slot, part(g)], c_r.at[slot, g])

        def body(f, carry):
            s = O[q, c, f].astype(jnp.float32) + PR[q, f].astype(jnp.float32)
            for slot in slots:
                s += RX[slot, f].astype(jnp.float32)
            O[q, c, f] = s.astype(jnp.bfloat16)
            return carry

        lax.fori_loop(g * NY, (g + 1) * NY, body, 0)

    def unit(q, g, up, has):
        n = z + toward if up else z - toward
        slot = jnp.where(jnp.logical_and(q == n, low if up else jnp.logical_not(low)), NZ, q)
        add_part(q, g, [q] if has else [])
        pass_on(q, g, slot, n).start()

    def column_block(g):
        columns(g)
        lax.fori_loop(0, NZ, lambda q, carry: (pair_copy(q, g).start(), carry)[1], 0)

    def some_columns(q, g):
        def body(k, carry):
            f = g * NY + k
            p = jnp.dot(H[pl.ds(pl.multiple_of(q * M, M), M)], WR[f], preferred_element_type=jnp.float32)
            O[q, :, f] = p.astype(jnp.bfloat16).reshape(2, R, DK)
            return carry

        lax.fori_loop(0, NY, body, 0)
        pair_copy(q, g).start()

    def norm_own():
        for u in range(TS):
            landed(t_view(z, c, u), t_r.at[z, c, u])
        if EARLY:
            norm_rows(z)

    def token_time(k, m):
        d = abs(m - k)
        return 28 + 6 * (0 < k < m) if d == 1 else 22 + 12 * d + k

    def hidden_time(k, q):
        return 50.0 if q == k else max(41.5, token_time(k, q) + 2.5) + 1.5

    def first_w(k, m):
        d = abs(m - k)
        if d == 1:
            return 38 if m < k or k == 0 else 53
        return (60 if k == 0 else 62) + 6 * (d - 2)

    def second_w(k, m):
        d = abs(m - k)
        return (48.5 if m < k or k == 0 else 58) if d == 1 else first_w(k, m) + 6

    def columns_time(k, g):
        return (45.0 if k == 0 else 52.0) if g == k else second_w(k, g) + 5

    def unit_time(k, g, q):
        if k > 0:
            return unit_time(0, g, q) + 6 * k
        return max(columns_time(0, g), hidden_time(0, q)) + 3

    def program(k, up):
        ops = []

        def op(t, fn):
            ops.append((t, len(ops), fn))

        others = sorted((m for m in range(NZ) if m != k), key=lambda m: abs(m - k))
        op(0.2, lambda: first(E, z, True))
        op(0.3, lambda: own_tokens(k, up))
        op(5.5, lambda: second(E, z))
        op(6, norm_own)
        op(9 if k == 0 else 33, lambda: first(W, z, True))
        op(19 if k == 0 else 43.5, lambda: second(W, z))
        op(columns_time(k, k), lambda: landed(W.view(x, z, y), W.l.at[z]))
        op(columns_time(k, k), lambda: last(W, z))
        op(41, lambda: landed(E.view(x, z, y), E.l.at[z]))
        for m in range(NZ):
            op(41, lambda m=m: last(E, src(m)))
        for m in others:
            d, q = abs(m - k), src(m)
            mine = m > k if up else m < k
            if mine:
                op(0.22 + 0.01 * d, lambda q=q: along_line(E, q))
                sent = (37 if 0 < k < m else 0.4) if d == 1 else 45 + 0.1 * d
                op(sent, lambda q=q: along_line(W, q))
            else:
                op(0.1, lambda q=q: hand_over(E, q))
                op(0.15, lambda q=q: hand_over(W, q))
            t = token_time(k, m)
            comes = m < k if up else m > k
            if comes:
                op(t, lambda m=m: relay_tokens(k, m, up))
            else:
                op(t + 2.1, lambda q=q: take_tokens(q))
            if EARLY:
                op(t + 2.2, lambda q=q: norm_rows(q))
            e = 8.5 if d == 1 else 12 + 5 * d if k == 0 else 8.5 * d
            op(e, lambda q=q: first(E, q))
            op(min(33, e + (6.5 if k == 0 else 11.5)), lambda q=q: second(E, q))
            op(first_w(k, m), lambda q=q: first(W, q))
            op(second_w(k, m), lambda q=q: second(W, q))
            op(columns_time(k, m), lambda q=q: last(W, q))
        for m in range(NZ):
            op(hidden_time(k, m), lambda m=m: expand_rows(src(m)))
        latest = max(hidden_time(k, m) for m in range(NZ))
        ready = {}
        for g in range(NZ):
            if columns_time(k, g) >= latest:
                op(columns_time(k, g) + 0.1, lambda g=g: column_block(src(g)))
            for q in range(NZ - 1, -1, -1):
                ready[g, q] = max(columns_time(k, g), hidden_time(k, q)) + 0.1
                if columns_time(k, g) < latest:
                    op(ready[g, q], lambda g=g, q=q: some_columns(src(q), src(g)))
        for g in range(NZ):
            for q in range(NZ - 1, -1, -1):
                if q > k:
                    t = max(unit_time(k, g, q), ready[g, q] + 1)
                    op(t, lambda g=g, q=q: unit(src(q), src(g), True, k > 0))
                if q < k:
                    t = max(unit_time(NZ - 1 - k, NZ - 1 - g, NZ - 1 - q), ready[g, q] + 1)
                    op(t, lambda g=g, q=q: unit(src(q), src(g), False, True))
        for _, _, fn in sorted(ops, key=lambda o: o[:2]):
            fn()

    own = [pltpu.make_async_copy(t_src, t_view(z, c, u), t_r.at[z, c, u])
           for u, t_src in ((u, tok.at[pl.ds(u * RT, RT)]) for u in range(TS))]
    own += [pltpu.make_async_copy(E.piece(z), E.view(x, z, y), E.l.at[z]),
            pltpu.make_async_copy(W.piece(z), W.view(x, z, y), W.l.at[z])]
    for copy in own:
        copy.start()
    for k in range((NZ + 1) // 2):
        pl.when(jnp.logical_and(mz == k, lifts))(functools.partial(program, k, True))
        pl.when(jnp.logical_and(mz == k, jnp.logical_not(lifts)))(functools.partial(program, k, False))

    def finish(g, carry):
        pl.when(jnp.logical_and(z > 0, z < NZ - 1))(lambda: add_part(z, g, [z, NZ]))
        pl.when(z == 0)(lambda: add_part(z, g, [z]))
        pl.when(z == NZ - 1)(lambda: add_part(z, g, [NZ]))
        return carry

    lax.fori_loop(0, NZ, finish, 0)

    def squares(f, acc):
        m = O[z, c, f].astype(jnp.float32)
        return acc + jnp.sum(m * m, axis=-1, keepdims=True)

    total = lax.fori_loop(0, NZ * NY, squares, jnp.zeros((R, 1), jnp.float32))
    scale = lax.rsqrt(total / D + NORM_EPS)
    for f in range(NZ * NY):
        cols = slice(f * DK, (f + 1) * DK)
        out[:, cols] = (O[z, c, f].astype(jnp.float32) * scale * gain_out[:, cols]).astype(jnp.bfloat16)

    drain_weight(E)
    drain_weight(W)

    def drain(q, carry):
        m = src(q)
        for u in range(TS):
            for cc in (0, 1):
                v = t_view(q, cc, u)
                pl.when(jnp.where(q == z, c == cc, jnp.where(lifts, m < mz, m > mz)))(
                    lambda: rc(v, v, t_ps.at[q, cc, u], t_r.at[q, cc, u], peer).wait_send())
                pl.when(jnp.where(lifts, jnp.logical_and(m <= mz, NZ > 1), jnp.logical_and(m >= mz, mz > 0)))(
                    lambda: rc(v, v, t_ls.at[q, cc, u], t_r.at[q, cc, u], peer).wait_send())
        for g in range(NZ):
            pair_copy(q, g).wait_send()
            pl.when(q != z)(lambda: pass_on(q, g, q, z).wait_send())
        return carry

    lax.fori_loop(0, NZ, drain, 0)


def per_device(FS, TP, tokens, pre_gain, w_expand, w_reduce, post_gain):
    NX = TP // 2
    NY = max(k for k in range(1, FS + 1) if FS % k == 0 and (k == 1 or 2 * k * k <= FS))
    NZ = FS // NY
    R, D = tokens.shape
    DK, F = w_expand.shape
    H4 = F // NZ
    bf = jnp.bfloat16
    dma = pltpu.SemaphoreType.DMA
    mx = max(NX, NY)
    early = 2 * NZ * R * D * 2 <= 8 * 1024 * 1024
    vmem = pl.BlockSpec(memory_space=pltpu.VMEM)
    hbm = pl.BlockSpec(memory_space=pl.ANY)
    return pl.pallas_call(
        functools.partial(kernel, NX, NY, NZ, early),
        out_shape=jax.ShapeDtypeStruct((R, D), bf),
        in_specs=[hbm, vmem, hbm, hbm, vmem],
        out_specs=vmem,
        scratch_shapes=[
            pltpu.VMEM((NZ, 2, R, D), bf),
            pltpu.VMEM(((NZ if early else 1) * 2 * R, D), bf),
            pltpu.VMEM((NX, D, H4), bf),
            pltpu.VMEM((FS, NX * H4, DK), bf),
            pltpu.VMEM((NZ, DK, H4), bf),
            pltpu.VMEM((NZ, H4, DK), bf),
            pltpu.VMEM((NZ * 2 * R, NX * H4), bf),
            pltpu.VMEM((NZ, 2, FS, R, DK), bf),
            pltpu.VMEM((NZ, FS, R, DK), bf),
            pltpu.VMEM((NZ + 1, FS, R, DK), bf),
            dma((NZ, 2, TS)), dma((NZ, 2, TS)), dma((NZ, 2, TS)),
            dma((NZ,)), dma((NZ, mx, 2)), dma((NZ, mx, mx, 2)), dma((NZ,)), dma((NX, NZ, NY, 2)), dma((NZ,)), dma((NZ,)),
            dma((NZ,)), dma((NZ, mx, 2)), dma((NZ, mx, mx, 2)), dma((NZ,)), dma((NX, NZ, NY, 2)), dma((NZ,)), dma((NZ,)),
            dma((NZ, NZ)), dma((NZ, NZ)), dma((NZ, NZ)), dma((NZ + 1, NZ)),
        ],
        compiler_params=pltpu.CompilerParams(
            collective_id=0, has_side_effects=True, vmem_limit_bytes=64 * 1024 * 1024 - 128 * 1024),
    )(tokens, pre_gain.reshape(1, D), w_expand, w_reduce, post_gain.reshape(1, D))


def solution(mesh):
    return jax.shard_map(
        functools.partial(per_device, mesh.shape["fs"], mesh.shape["tp"]),
        mesh=mesh,
        in_specs=(P(("fs", "tp"), None), P(), P("fs", "tp"), P("tp", "fs"), P()),
        out_specs=P(("fs", "tp"), None),
        check_vma=False,
    )
```

```python
import functools

import jax
import jax.numpy as jnp
from jax import lax
from jax.experimental import pallas as pl
from jax.experimental.pallas import tpu as pltpu
from jax.sharding import PartitionSpec as P

NORM_EPS = 1e-06
MESH = pl.DeviceIdType.MESH
TS = 2


def kernel(NX, NY, NZ, EARLY, tok, gain_in, w_e, w_r, gain_out, out,
           TG, N, WE, WR, XE, XR, H, O, PR, RX,
           t_ls, t_ps, t_r, e_a, e_b, e_c, e_l, e_r, e_x, e_y, r_a, r_b, r_c, r_l, r_r, r_x, r_y, p_s, p_r, c_s, c_r):
    R, D = tok.shape
    DK, F = w_e.shape
    H4 = F // NZ
    RT = R // TS
    fs, tp = lax.axis_index("fs"), lax.axis_index("tp")
    z, y = fs // NY, fs % NY
    x, c = tp // 2, tp % 2
    pc = 1 - c
    peer = (fs, x * 2 + pc)

    low = 2 * z < NZ
    mz = jnp.where(low, z, NZ - 1 - z)
    toward = jnp.where(low, 1, -1)
    lifts = c == jnp.where(low, 1, 0)

    def src(m):
        return jnp.where(low, m, NZ - 1 - m)

    def zdev(q):
        return (q * NY + y, tp)

    xs = [(x + j) % NX for j in range(1, NX)]
    ys = [(y + j) % NY for j in range(1, NY)]
    xdevs = [(fs, q * 2 + c) for q in xs]
    ydevs = [(z * NY + q, tp) for q in ys]

    barrier = pltpu.get_barrier_semaphore()
    others = [zdev((z + j) % NZ) for j in range(1, NZ)] + xdevs + ydevs + [peer]
    for dev in others:
        pl.semaphore_signal(barrier, inc=1, device_id=dev, device_id_type=MESH)
    pl.semaphore_wait(barrier, len(others))

    def rc(src, dst, ss, rs, dev):
        return pltpu.make_async_remote_copy(src_ref=src, dst_ref=dst, send_sem=ss, recv_sem=rs,
                                            device_id=dev, device_id_type=MESH)

    def landed(ref, sem):
        pltpu.make_async_copy(ref, ref, sem).wait()

    def rows_of(start, size, half):
        if half is None:
            return pl.ds(pl.multiple_of(start, size), size)
        return pl.ds(pl.multiple_of(start + half * (size // 2), size // 2), size // 2)

    def e_view(xq, zq, yq, half=None):
        return WE.at[xq, rows_of((zq * NY + yq) * DK, DK, half)]

    def r_view(xq, zq, yq, half=None):
        return WR.at[zq * NY + yq, rows_of(xq * H4, H4, half)]

    def e_piece(q, half=None):
        cols = pl.ds(pl.multiple_of(q * H4, H4), H4)
        return w_e.at[:, cols] if half is None else w_e.at[rows_of(0, DK, half), cols]

    def r_piece(q, half=None):
        return w_r.at[rows_of(q * H4, H4, half)]

    class Weight:
        def __init__(self, view, piece, held, a, b, cc, l, r, sx, rx):
            self.view, self.piece, self.held, self.a, self.b, self.c = view, piece, held, a, b, cc
            self.l, self.r, self.sx, self.rx = l, r, sx, rx

    E = Weight(e_view, e_piece, XE, e_a, e_b, e_c, e_l, e_r, e_x, e_y)
    W = Weight(r_view, r_piece, XR, r_a, r_b, r_c, r_l, r_r, r_x, r_y)
    ways = ((xdevs, xs, ydevs, ys), (ydevs, ys, xdevs, xs))

    def hand_over(w, q):
        rc(w.piece(q), w.held.at[q], w.a.at[q], w.rx.at[q], peer).start()

    def along_line(w, q):
        rc(w.piece(q), w.view(x, z, y), w.a.at[q], w.l.at[z], zdev(q)).start()
        landed(w.held.at[q], w.rx.at[q])
        rc(w.held.at[q], w.view(x, z, y), w.sx.at[q], w.l.at[z], (q * NY + y, x * 2 + pc)).start()

    def first(w, q, own=False):
        if not own:
            landed(w.view(x, q, y), w.l.at[q])
        for h in (0, 1):
            for j, dev in enumerate(ways[h][0]):
                rc(w.piece(q, h) if own else w.view(x, q, y, h), w.view(x, q, y, h), w.b.at[q, j, h],
                   w.r.at[x, q, y, h], dev).start()
        for h in (0, 1):
            for j, dev in enumerate(ways[h][2]):
                rc(w.piece(q, h) if own else w.view(x, q, y, h), w.view(x, q, y, h), w.c.at[q, 0, j, h],
                   w.r.at[x, q, y, h], dev).start()

    def second(w, q):
        for h in (0, 1):
            for i, m in enumerate(ways[h][1]):
                where = (m, q, y) if h == 0 else (x, q, m)
                landed(w.view(*where, h), w.r.at[(*where, h)])
                for j, dev in enumerate(ways[h][2]):
                    rc(w.view(*where, h), w.view(*where, h), w.c.at[q, 1 + i, j, h], w.r.at[(*where, h)], dev).start()

    def last(w, q):
        for h in (0, 1):
            for a in [x] + xs if h == 0 else xs:
                for b in ys if h == 0 else [y] + ys:
                    landed(w.view(a, q, b, h), w.r.at[a, q, b, h])

    def drain_weight(w):
        def body(q, carry):
            pl.when(q != z)(lambda: rc(w.piece(q), w.view(x, z, y), w.a.at[q], w.l.at[z], peer).wait_send())
            pl.when(jnp.where(lifts, src(q) > mz, src(q) < mz))(
                lambda: rc(w.held.at[q], w.view(x, z, y), w.sx.at[q], w.l.at[z], peer).wait_send())
            for h in (0, 1):
                v = w.view(x, q, y, h)
                for j in range(len(ways[h][0])):
                    rc(v, v, w.b.at[q, j, h], w.r.at[x, q, y, h], peer).wait_send()
                for i in range(1 + len(ways[h][1])):
                    for j in range(len(ways[h][2])):
                        rc(v, v, w.c.at[q, i, j, h], w.r.at[x, q, y, h], peer).wait_send()
            return carry

        lax.fori_loop(0, NZ, body, 0)

    def t_view(q, cc, u):
        return TG.at[q, cc, pl.ds(u * RT, RT)]

    def send_tokens(source, q, cc, u, up):
        n = z + toward if up else z - toward
        dev = (n * NY + y, tp)
        rc(source, t_view(q, cc, u), t_ls.at[q, cc, u], t_r.at[q, cc, u], dev).start()

    def peer_tokens(source, q, cc, u):
        rc(source, t_view(q, cc, u), t_ps.at[q, cc, u], t_r.at[q, cc, u], peer).start()

    def relay_tokens(k, m, up):
        q = src(m)
        for u in range(TS):
            for cc in (0, 1):
                v = t_view(q, cc, u)
                landed(v, t_r.at[q, cc, u])
                if up or k > 0:
                    send_tokens(v, q, cc, u, up)
                peer_tokens(v, q, cc, u)

    def own_tokens(k, up):
        for u in range(TS):
            peer_tokens(tok.at[pl.ds(u * RT, RT)], z, c, u)
        linked = NZ > 1 and (up or k > 0)
        if linked:
            for u in range(TS):
                send_tokens(tok.at[pl.ds(u * RT, RT)], z, c, u, up)
        for u in range(TS):
            landed(t_view(z, pc, u), t_r.at[z, pc, u])
            if linked:
                send_tokens(t_view(z, pc, u), z, pc, u, up)

    def take_tokens(q):
        for u in range(TS):
            for cc in (0, 1):
                landed(t_view(q, cc, u), t_r.at[q, cc, u])

    M = 2 * R
    sub = 32

    def norm_rows(q):
        base = q * M if EARLY else 0

        def norm(i, carry):
            v = TG[q, i // (R // sub), pl.ds(pl.multiple_of((i % (R // sub)) * sub, sub), sub)].astype(jnp.float32)
            v = v * lax.rsqrt(jnp.mean(v * v, axis=-1, keepdims=True) + NORM_EPS) * gain_in[...]
            N[pl.ds(pl.multiple_of(base + i * sub, sub), sub)] = v.astype(jnp.bfloat16)
            return carry

        lax.fori_loop(0, M // sub, norm, 0)

    def expand_rows(q):
        if not EARLY:
            norm_rows(q)
        rows = pl.ds(pl.multiple_of(q * M, M), M)
        src = rows if EARLY else slice(None)
        for i in range(NX):
            p = jnp.dot(N[src], WE[i], preferred_element_type=jnp.float32)
            H[rows, i * H4:(i + 1) * H4] = jnp.square(jnp.maximum(p, 0.0)).astype(jnp.bfloat16)

    def part(g):
        return pl.ds(g * NY, NY)

    def pair_copy(q, g):
        return rc(O.at[q, pc, part(g)], PR.at[q, part(g)], p_s.at[g, q], p_r.at[g, q], peer)

    def pass_on(q, g, slot, n):
        return rc(O.at[q, c, part(g)], RX.at[slot, part(g)], c_s.at[q, g], c_r.at[slot, g], zdev(n))

    def add_part(q, g, slots):
        landed(PR.at[q, part(g)], p_r.at[g, q])
        for slot in slots:
            landed(RX.at[slot, part(g)], c_r.at[slot, g])

        def body(f, carry):
            s = O[q, c, f].astype(jnp.float32) + PR[q, f].astype(jnp.float32)
            for slot in slots:
                s += RX[slot, f].astype(jnp.float32)
            O[q, c, f] = s.astype(jnp.bfloat16)
            return carry

        lax.fori_loop(g * NY, (g + 1) * NY, body, 0)

    def unit(q, g, up, has):
        n = z + toward if up else z - toward
        slot = jnp.where(jnp.logical_and(q == n, low if up else jnp.logical_not(low)), NZ, q)
        add_part(q, g, [q] if has else [])
        pass_on(q, g, slot, n).start()

    def some_columns(q, g):
        def body(k, carry):
            f = g * NY + k
            p = jnp.dot(H[pl.ds(pl.multiple_of(q * M, M), M)], WR[f], preferred_element_type=jnp.float32)
            O[q, :, f] = p.astype(jnp.bfloat16).reshape(2, R, DK)
            return carry

        lax.fori_loop(0, NY, body, 0)
        pair_copy(q, g).start()

    def norm_own():
        for u in range(TS):
            landed(t_view(z, c, u), t_r.at[z, c, u])
        if EARLY:
            norm_rows(z)

    def token_time(k, m):
        d = abs(m - k)
        return 28 + 6 * (0 < k < m) if d == 1 else 26 + 11.5 * d + k

    def hidden_time(k, q):
        return 50.0 if q == k else max(41.5, token_time(k, q) + 2.5) + 1.5

    def first_w(k, m):
        d = abs(m - k)
        if k == 0:
            return 38 if d == 1 else 56 + 13 * (d - 2)
        return 38 if d == 1 and m < k else 56 if d == 1 else 61.8 + 10 * (d - 2)

    def second_w(k, m):
        d = abs(m - k)
        if k == 0:
            return 46 if d == 1 else 61 + 13.5 * (d - 2)
        return 47 if d == 1 and m < k else 62 if d == 1 else 66 + 10 * (d - 2)

    def columns_time(k, g):
        return (45.0 if k == 0 else 52.0) if g == k else second_w(k, g) + 5

    def unit_time(k, g, q):
        if k > 0:
            return unit_time(0, g, q) + 6 * k
        return max(columns_time(0, g), hidden_time(0, q)) + 3

    def program(k, up):
        ops = []

        def op(t, fn):
            ops.append((t, len(ops), fn))

        others = sorted((m for m in range(NZ) if m != k), key=lambda m: abs(m - k))
        op(0.2, lambda: first(E, z, True))
        op(0.3, lambda: own_tokens(k, up))
        op(5.5, lambda: second(E, z))
        op(6, norm_own)
        op(9 if k == 0 else 33, lambda: first(W, z, True))
        op(19 if k == 0 else 43.5, lambda: second(W, z))
        op(columns_time(k, k), lambda: landed(W.view(x, z, y), W.l.at[z]))
        op(columns_time(k, k), lambda: last(W, z))
        op(41, lambda: landed(E.view(x, z, y), E.l.at[z]))
        for m in range(NZ):
            op(41, lambda m=m: last(E, src(m)))
        for m in others:
            d, q = abs(m - k), src(m)
            mine = m > k if up else m < k
            if mine:
                op(0.22 + 0.01 * d, lambda q=q: along_line(E, q))
                sent = (37 if 0 < k < m else 0.4) if d == 1 else 36.9 if k > 0 else 52.9 - 0.1 * d
                op(sent, lambda q=q: along_line(W, q))
            else:
                op(0.1, lambda q=q: hand_over(E, q))
                op(0.15, lambda q=q: hand_over(W, q))
            t = token_time(k, m)
            comes = m < k if up else m > k
            if comes:
                op(t, lambda m=m: relay_tokens(k, m, up))
            else:
                op(t + 2.1, lambda q=q: take_tokens(q))
            if EARLY:
                op(t + 2.2, lambda q=q: norm_rows(q))
            e = 8.5 if d == 1 else 12 + 5 * d if k == 0 else 8.5 * d
            op(e, lambda q=q: first(E, q))
            op(min(33, e + (6.5 if k == 0 else 11.5)), lambda q=q: second(E, q))
            op(first_w(k, m), lambda q=q: first(W, q))
            op(second_w(k, m), lambda q=q: second(W, q))
            op(columns_time(k, m), lambda q=q: last(W, q))
        for m in range(NZ):
            op(hidden_time(k, m), lambda m=m: expand_rows(src(m)))
        ready = {}
        for g in range(NZ):
            for q in sorted(range(NZ), key=lambda q: -abs(q - k)):
                ready[g, q] = max(columns_time(k, g), hidden_time(k, q)) + 0.1
                op(ready[g, q], lambda g=g, q=q: some_columns(src(q), src(g)))
        for g in range(NZ):
            for q in range(NZ - 1, -1, -1):
                if q > k:
                    t = max(unit_time(k, g, q), ready[g, q] + 1)
                    op(t, lambda g=g, q=q: unit(src(q), src(g), True, k > 0))
                if q < k:
                    t = max(unit_time(NZ - 1 - k, NZ - 1 - g, NZ - 1 - q), ready[g, q] + 1)
                    op(t, lambda g=g, q=q: unit(src(q), src(g), False, True))
        for _, _, fn in sorted(ops, key=lambda o: o[:2]):
            fn()

    own = [pltpu.make_async_copy(t_src, t_view(z, c, u), t_r.at[z, c, u])
           for u, t_src in ((u, tok.at[pl.ds(u * RT, RT)]) for u in range(TS))]
    own += [pltpu.make_async_copy(E.piece(z), E.view(x, z, y), E.l.at[z]),
            pltpu.make_async_copy(W.piece(z), W.view(x, z, y), W.l.at[z])]
    for copy in own:
        copy.start()
    for k in range((NZ + 1) // 2):
        pl.when(jnp.logical_and(mz == k, lifts))(functools.partial(program, k, True))
        pl.when(jnp.logical_and(mz == k, jnp.logical_not(lifts)))(functools.partial(program, k, False))

    drain_weight(E)
    drain_weight(W)

    def drain(q, carry):
        m = src(q)
        for u in range(TS):
            for cc in (0, 1):
                v = t_view(q, cc, u)
                pl.when(jnp.where(q == z, c == cc, jnp.where(lifts, m < mz, m > mz)))(
                    lambda: rc(v, v, t_ps.at[q, cc, u], t_r.at[q, cc, u], peer).wait_send())
                pl.when(jnp.where(lifts, jnp.logical_and(m <= mz, NZ > 1), jnp.logical_and(m >= mz, mz > 0)))(
                    lambda: rc(v, v, t_ls.at[q, cc, u], t_r.at[q, cc, u], peer).wait_send())
        for g in range(NZ):
            pair_copy(q, g).wait_send()
            pl.when(q != z)(lambda: pass_on(q, g, q, z).wait_send())
        return carry

    lax.fori_loop(0, NZ, drain, 0)

    def finish(t, acc):
        g = jnp.where(low, NZ - 1 - t, t)
        landed(PR.at[z, part(g)], p_r.at[g, z])
        pl.when(z > 0)(lambda: landed(RX.at[NZ, part(g)], c_r.at[NZ, g]))
        pl.when(z < NZ - 1)(lambda: landed(RX.at[z, part(g)], c_r.at[z, g]))

        def body(f, acc):
            s = O[z, c, f].astype(jnp.float32) + PR[z, f].astype(jnp.float32)
            s += jnp.where(z < NZ - 1, RX[z, f].astype(jnp.float32), 0.0)
            s += jnp.where(z > 0, RX[NZ, f].astype(jnp.float32), 0.0)
            O[z, c, f] = s.astype(jnp.bfloat16)
            m = O[z, c, f].astype(jnp.float32)
            return acc + m * m

        return lax.fori_loop(g * NY, (g + 1) * NY, body, acc)

    squares = lax.fori_loop(0, NZ, finish, jnp.zeros((R, DK), jnp.float32))
    total = jnp.sum(squares, axis=-1, keepdims=True)
    scale = lax.rsqrt(total / D + NORM_EPS)
    for f in range(NZ * NY):
        cols = slice(f * DK, (f + 1) * DK)
        out[:, cols] = (O[z, c, f].astype(jnp.float32) * scale * gain_out[:, cols]).astype(jnp.bfloat16)


def per_device(FS, TP, tokens, pre_gain, w_expand, w_reduce, post_gain):
    NX = TP // 2
    NY = max(k for k in range(1, FS + 1) if FS % k == 0 and (k == 1 or 2 * k * k <= FS))
    NZ = FS // NY
    R, D = tokens.shape
    DK, F = w_expand.shape
    H4 = F // NZ
    bf = jnp.bfloat16
    dma = pltpu.SemaphoreType.DMA
    mx = max(NX, NY)
    early = 2 * NZ * R * D * 2 <= 8 * 1024 * 1024
    vmem = pl.BlockSpec(memory_space=pltpu.VMEM)
    hbm = pl.BlockSpec(memory_space=pl.ANY)
    return pl.pallas_call(
        functools.partial(kernel, NX, NY, NZ, early),
        out_shape=jax.ShapeDtypeStruct((R, D), bf),
        in_specs=[hbm, vmem, hbm, hbm, vmem],
        out_specs=vmem,
        scratch_shapes=[
            pltpu.VMEM((NZ, 2, R, D), bf),
            pltpu.VMEM(((NZ if early else 1) * 2 * R, D), bf),
            pltpu.VMEM((NX, D, H4), bf),
            pltpu.VMEM((FS, NX * H4, DK), bf),
            pltpu.VMEM((NZ, DK, H4), bf),
            pltpu.VMEM((NZ, H4, DK), bf),
            pltpu.VMEM((NZ * 2 * R, NX * H4), bf),
            pltpu.VMEM((NZ, 2, FS, R, DK), bf),
            pltpu.VMEM((NZ, FS, R, DK), bf),
            pltpu.VMEM((NZ + 1, FS, R, DK), bf),
            dma((NZ, 2, TS)), dma((NZ, 2, TS)), dma((NZ, 2, TS)),
            dma((NZ,)), dma((NZ, mx, 2)), dma((NZ, mx, mx, 2)), dma((NZ,)), dma((NX, NZ, NY, 2)), dma((NZ,)), dma((NZ,)),
            dma((NZ,)), dma((NZ, mx, 2)), dma((NZ, mx, mx, 2)), dma((NZ,)), dma((NX, NZ, NY, 2)), dma((NZ,)), dma((NZ,)),
            dma((NZ, NZ)), dma((NZ, NZ)), dma((NZ, NZ)), dma((NZ + 1, NZ)),
        ],
        compiler_params=pltpu.CompilerParams(
            collective_id=0, has_side_effects=True, vmem_limit_bytes=64 * 1024 * 1024 - 128 * 1024),
    )(tokens, pre_gain.reshape(1, D), w_expand, w_reduce, post_gain.reshape(1, D))


def solution(mesh):
    return jax.shard_map(
        functools.partial(per_device, mesh.shape["fs"], mesh.shape["tp"]),
        mesh=mesh,
        in_specs=(P(("fs", "tp"), None), P(), P("fs", "tp"), P("tp", "fs"), P()),
        out_specs=P(("fs", "tp"), None),
        check_vma=False,
    )
```
